32 devices in a mesh: sp: 8 (over z, y), tp: 4 (over x, core).
Axes of the slice: x: 2, y: 2, z: 4, core: 2. Of those that a mesh axis runs over, the one named last changes fastest.
Arguments:
- query_proj: bfloat16 [2048, 2048], P('sp', 'tp'), may hold values from -240 to 240
- key_projection: bfloat16 [2048, 512], P('sp', 'tp'), may hold values from -6 to 6
- value_projection: bfloat16 [2048, 512], P('sp', 'tp'), may hold values from -6 to 6
- sink_logit: float32 [32], P('tp'), may hold values from 1 to 6
- residual: bfloat16 [2048, 2048], P('sp'), may hold values from -3 to 3
- w_out: bfloat16 [2048, 2048], P('tp'), may hold values from -1 to 1
- norm_gain: float32 [2048], replicated, may hold values from 0.1 to 1.9
- routes: int32 [2048, 2], P('sp'), may hold values from 0 to 7, all different within a row; in each aligned block of 256 rows (0 to 255, 256 to 511, ...) at most 128 rows name the same one
- route_weights: float32 [2048, 2], P('sp'), may hold values from 0.1 to 1
- w_gate: bfloat16 [8, 2048, 2560], P('sp', None, 'tp'), may hold values from -0.125 to 0.125
- w_up: bfloat16 [8, 2048, 2560], P('sp', None, 'tp'), may hold values from -0.125 to 0.125
- w_down: bfloat16 [8, 2560, 2048], P('sp', 'tp'), may hold values from -0.125 to 0.125
Outputs:
- layer_out: bfloat16 [2048, 2048], P('sp', 'tp')
The draws below stay inside these ranges and needn't reach their ends.
Inputs may be any that keep to these rules, and one draw needn't show every extreme that they name: `routes`: within the rows of one index of sp (aligned blocks of 256 tokens), no expert is named more than 128 times, and in some block one expert is named exactly 128 times. The two experts of a token differ.
All inputs are finite; a program needn't handle non-finite values.
Results may differ from the reference program's by a relative error of at most 0.015.
Values may be sent and summed in bfloat16 or wider, within the bound.
A program may use at most 64 MiB of HBM per device.

```python
import math
import jax
import jax.numpy as jnp
import numpy as np
from jax import lax

D = 2048
QUERY_HEADS = 32
KEY_VALUE_HEADS = 8
HEAD_SIZE = 64
WINDOW = 128
GRID_W = 64
EF = 2560
TOP = 2
TOK_DEV = 256
SEQUENCE_TOKENS = 2048
EXPERTS = 8
CAP = 128
WIDTH_BLOCKS = 4
N_SP = 8


def drawn_pair(key):
    unrotated_keys = jnp.clip(jax.random.normal(jax.random.fold_in(key, 11), (SEQUENCE_TOKENS, KEY_VALUE_HEADS, HEAD_SIZE), jnp.float32), -6.0, 6.0)
    unrotated_queries = jnp.clip(jax.random.normal(jax.random.fold_in(key, 12), (SEQUENCE_TOKENS, QUERY_HEADS, HEAD_SIZE), jnp.float32), -6.0, 6.0)
    return (unrotated_queries.reshape(SEQUENCE_TOKENS, QUERY_HEADS * HEAD_SIZE), unrotated_keys.reshape(SEQUENCE_TOKENS, KEY_VALUE_HEADS * HEAD_SIZE))


def draw_query_proj(key, part):
    return drawn_pair(key)[0].astype(jnp.bfloat16)


def draw_key_projection(key, part):
    return drawn_pair(key)[1].astype(jnp.bfloat16)


def block_scale(rng, extent, cuts, low, top_value):
    loudness, own = 1.0, jax.random.fold_in(rng, 6)
    for dim, parts in cuts:
        heights = jnp.exp(jax.random.uniform(jax.random.fold_in(own, dim), (parts,), jnp.float32, low / len(cuts), top_value / len(cuts)))
        loudness = loudness * jnp.repeat(heights, extent[dim] // parts).reshape([-1 if axis == dim else 1 for axis in range(len(extent))])
    return loudness


def routed_block(rng, own, number, rows, count, top, most, lean):
    order = jax.random.permutation(rng, count)
    crowded, usual = portions_of(count, rows * top, most, lean, True), portions_of(count, rows * top, most, lean, False)
    places = jnp.arange(count)

    def named(sizes, turn):
        used = int((sizes > 0).sum())
        fixed = max(1, used // 4)
        moved = fixed + (places - fixed + turn * (used - fixed)) % max(1, count - fixed)
        return jnp.zeros((count,), jnp.int32).at[order[jnp.where(places < fixed, places, moved)]].set(jnp.asarray(sizes, jnp.int32))

    sizes = jnp.where(number % 4 == 0, named(crowded, number // 4), named(usual, number - number // 4 - 1))
    mixed = jax.random.permutation(jax.random.fold_in(own, 3), count)
    giver, taker = mixed[0:count // 2 * 2:2], mixed[1:count // 2 * 2:2]
    margin = jnp.minimum(sizes[giver] - 1, most - sizes[taker]) // 2
    margin = jnp.where((giver == order[0]) | (taker == order[0]) | (sizes[taker] == 0), 0, jnp.maximum(margin, 0))
    moved = jax.random.randint(jax.random.fold_in(own, 4), (count // 2,), 0, 1 << 20) % (margin + 1)
    sizes = sizes.at[giver].add(-moved).at[taker].add(moved)
    items = jnp.searchsorted(jnp.cumsum(sizes), jnp.arange(rows * top), side="right").astype(jnp.int32)
    listing = items.reshape(top, rows).T
    listing = listing[jax.random.permutation(jax.random.fold_in(own, 1), rows)]
    turn = jax.random.randint(jax.random.fold_in(own, 2), (rows, 1), 0, top)
    return jnp.take_along_axis(listing, (jnp.arange(top)[None, :] + turn) % top, axis=1)


def portions_of(amount, total, limit, lean, full):
    loads = [(1 << 20) // math.isqrt(grade ** lean) + 1 for grade in range(1, amount + 1)]
    largest = limit if full else min(limit, max(-(-total // amount), total * loads[0] // sum(loads)))
    least = 1 if total - largest >= amount - 1 else 0
    counts, rest = [largest] + [least] * (amount - 1), total - largest - least * (amount - 1)
    while rest > 0:
        free = [i for i in range(1, amount) if counts[i] < largest] or [i for i in range(1, amount) if counts[i] < limit]
        mass, budget = sum([loads[i] for i in free]), rest
        for i in free:
            extra = min(limit - counts[i], max(1, budget * loads[i] // mass), rest)
            counts[i] = counts[i] + extra
            rest = rest - extra
    return np.array(counts)


def scatter_about(key, dims, spread, reach, cuts=(), held_as=jnp.bfloat16):
    loudness = block_scale(key, dims, cuts, -0.22, 0.18) if cuts else 1.0
    array = jax.random.normal(key, dims, jnp.float32) * spread * loudness
    return jnp.minimum(jnp.maximum(array, -reach), reach).astype(held_as)


def setup_inputs(seed: int = 0) -> dict:
    key_list = jax.random.split(jax.random.key(seed), 13)
    query_proj = draw_query_proj(jax.random.fold_in(key_list[12], 71), 0)
    key_projection = draw_key_projection(jax.random.fold_in(key_list[12], 71), 0)
    value_projection = scatter_about(key_list[2], (SEQUENCE_TOKENS, KEY_VALUE_HEADS * HEAD_SIZE), 1.0, 6.0, ((0, 8), (1, 4)))
    sink_logit = jnp.clip(1.0 + 5.0 * jax.random.uniform(key_list[3], (QUERY_HEADS,), jnp.float32) ** block_scale(key_list[3], (QUERY_HEADS,), ((0, 4),), -0.2, 0.2), 1.0, 6.0)
    residual = scatter_about(key_list[4], (SEQUENCE_TOKENS, D), 0.5, 3.0, ((0, 8),))
    w_out = scatter_about(key_list[5], (QUERY_HEADS * HEAD_SIZE, D), (QUERY_HEADS * HEAD_SIZE // 64) ** -0.5, 1.0, ((0, 4),))
    norm_gain = jnp.clip(1.0 + 0.18 * jax.random.normal(key_list[6], (D,), jnp.float32), 0.1, 1.9)
    routes_keys = jax.random.split(jax.random.fold_in(key_list[7], 1), SEQUENCE_TOKENS // TOK_DEV)
    routes_turns = jax.random.permutation(jax.random.fold_in(key_list[7], 3), SEQUENCE_TOKENS // TOK_DEV)
    routes = jax.vmap(lambda own, number: routed_block(jax.random.fold_in(key_list[7], 2), own, number, TOK_DEV, EXPERTS, TOP, CAP, 2))(routes_keys, routes_turns).reshape((SEQUENCE_TOKENS, TOP))
    route_weights = jnp.clip(jnp.exp(math.log(1.0) - 2.3025851 * jax.random.uniform(key_list[8], (SEQUENCE_TOKENS, TOP), jnp.float32) ** block_scale(key_list[8], (SEQUENCE_TOKENS, TOP), ((0, 8),), -0.2, 0.2)), 0.1, 1.0)
    w_gate = scatter_about(key_list[9], (EXPERTS, D, EF), D ** -0.5, 0.125, ((0, 8), (2, 4)))
    w_up = scatter_about(key_list[10], (EXPERTS, D, EF), D ** -0.5, 0.125, ((0, 8), (2, 4)))
    w_down = scatter_about(key_list[11], (EXPERTS, EF, D), EF ** -0.5, 0.125, ((0, 8), (1, 4)))
    return dict(query_proj=query_proj, key_projection=key_projection, value_projection=value_projection, sink_logit=sink_logit, residual=residual, w_out=w_out, norm_gain=norm_gain, routes=routes, route_weights=route_weights, w_gate=w_gate, w_up=w_up, w_down=w_down)


ROPE_BASE = 10000.0
NORM_EPS = 1e-06

def rotate_pair(values_half, angles):
    first_half, second = jnp.split(values_half, 2, axis=-1)
    cosine = jnp.cos(angles)[:, None, :]
    sine_part = jnp.sin(angles)[:, None, :]
    return jnp.concatenate([first_half * cosine - second * sine_part, second * cosine + first_half * sine_part], axis=-1)

def axial_rotation(heads_in, token_positions):
    half_dim = HEAD_SIZE // 2
    inverse = ROPE_BASE ** (-jnp.arange(0, half_dim, 2, dtype=jnp.float32) / half_dim)
    row_angles = (token_positions // GRID_W).astype(jnp.float32)[:, None] * inverse
    col_angles = (token_positions % GRID_W).astype(jnp.float32)[:, None] * inverse
    as_float = heads_in.astype(jnp.float32)
    return jnp.concatenate([rotate_pair(as_float[..., :half_dim], row_angles), rotate_pair(as_float[..., half_dim:], col_angles)], axis=-1)

def attend_block(query_rows, key_rows, value_rows, sink_logit, query_pos, key_pos, total_rows):
    kv_heads = key_rows.shape[1]
    groups = query_rows.shape[1] // kv_heads
    grouped = query_rows.reshape(query_rows.shape[0], kv_heads, groups, HEAD_SIZE).astype(jnp.float32)
    scores = jnp.einsum('qkgd,jkd->kgqj', grouped, key_rows.astype(jnp.float32)) * HEAD_SIZE ** (-0.5)
    in_window = (jnp.abs(key_pos[None, :] - query_pos[:, None]) <= WINDOW) & (key_pos[None, :] >= 0) & (key_pos[None, :] < total_rows)
    scores = jnp.where(in_window[None, None], scores, -jnp.inf)
    sink_col = sink_logit.astype(jnp.float32).reshape(kv_heads, groups, 1, 1)
    largest = jnp.maximum(lax.optimization_barrier(jnp.max(scores, axis=-1, keepdims=True)), sink_col)
    exp_scores = jnp.exp(scores - largest)
    denominator = lax.optimization_barrier(jnp.sum(exp_scores, axis=-1, keepdims=True)) + jnp.exp(sink_col - largest)
    weights_bf = (exp_scores / denominator).astype(jnp.bfloat16)
    mixed_heads = jnp.einsum('kgqj,jkd->qkgd', weights_bf.astype(jnp.float32), value_rows.astype(jnp.float32))
    return mixed_heads.astype(jnp.bfloat16).reshape(query_rows.shape[0], -1)

def blocked_product(left, right, blocks_count):
    part_width = left.shape[1] // blocks_count
    accumulated = jnp.zeros((left.shape[0], right.shape[1]), jnp.float32)
    for block_number in range(blocks_count):
        partial_term = jnp.dot(left[:, block_number * part_width:(block_number + 1) * part_width], right[block_number * part_width:(block_number + 1) * part_width], preferred_element_type=jnp.float32).astype(jnp.bfloat16)
        accumulated = accumulated + lax.optimization_barrier(partial_term).astype(jnp.float32)
    return accumulated

def reference(query_proj, key_projection, value_projection, sink_logit, residual, w_out, norm_gain, routes, route_weights, w_gate, w_up, w_down):
    token_positions = jnp.arange(SEQUENCE_TOKENS, dtype=jnp.int32)
    rot_q = axial_rotation(query_proj.reshape(SEQUENCE_TOKENS, QUERY_HEADS, HEAD_SIZE), token_positions).astype(jnp.bfloat16)
    rotated_keys = axial_rotation(key_projection.reshape(SEQUENCE_TOKENS, KEY_VALUE_HEADS, HEAD_SIZE), token_positions).astype(jnp.bfloat16)
    value_head_rows = value_projection.reshape(SEQUENCE_TOKENS, KEY_VALUE_HEADS, HEAD_SIZE)
    pad_keys = jnp.pad(rotated_keys, ((WINDOW, WINDOW), (0, 0), (0, 0)))
    pad_values = jnp.pad(value_head_rows, ((WINDOW, WINDOW), (0, 0), (0, 0)))

    def one_block(block_index):
        block_start = (block_index * TOK_DEV).astype(jnp.int32)
        query_rows = lax.dynamic_slice_in_dim(rot_q, block_start, TOK_DEV, 0)
        key_rows = lax.dynamic_slice_in_dim(pad_keys, block_start, TOK_DEV + 2 * WINDOW, 0)
        value_rows = lax.dynamic_slice_in_dim(pad_values, block_start, TOK_DEV + 2 * WINDOW, 0)
        query_pos = block_start + jnp.arange(TOK_DEV, dtype=jnp.int32)
        key_pos = block_start - WINDOW + jnp.arange(TOK_DEV + 2 * WINDOW, dtype=jnp.int32)
        return attend_block(query_rows, key_rows, value_rows, sink_logit, query_pos, key_pos, SEQUENCE_TOKENS)
    attended = lax.map(one_block, jnp.arange(SEQUENCE_TOKENS // TOK_DEV, dtype=jnp.int32)).reshape(SEQUENCE_TOKENS, QUERY_HEADS * HEAD_SIZE)
    summed = blocked_product(attended, w_out, WIDTH_BLOCKS)
    stream = (residual.astype(jnp.float32) + summed).astype(jnp.bfloat16)
    as_float = stream.astype(jnp.float32)
    normed = (as_float * lax.rsqrt(lax.optimization_barrier(jnp.mean(as_float * as_float, axis=-1, keepdims=True)) + NORM_EPS) * norm_gain).astype(jnp.bfloat16)
    flat_routes = routes.reshape(N_SP, TOK_DEV * TOP)
    onehot = (flat_routes[:, :, None] == jnp.arange(EXPERTS, dtype=jnp.int32)[None, None, :]).astype(jnp.int32)
    slot_number = lax.optimization_barrier(jnp.sum(jnp.cumsum(onehot, axis=1) * onehot, axis=2)) - 1
    source = jnp.arange(N_SP, dtype=jnp.int32)[:, None]
    destination = (flat_routes * (N_SP * CAP) + source * CAP + slot_number).reshape(-1).astype(jnp.int32)
    copies = jnp.repeat(normed, TOP, axis=0)
    buffer = jnp.zeros((EXPERTS * N_SP * CAP, D), jnp.bfloat16).at[destination].set(copies)
    buffer = buffer.reshape(EXPERTS, N_SP * CAP, D)

    def expert(operands):
        expert_rows, gate_weight, up_weight, down_weight = operands
        gate_part = jnp.dot(expert_rows, gate_weight, preferred_element_type=jnp.float32)
        up_part = jnp.dot(expert_rows, up_weight, preferred_element_type=jnp.float32)
        hidden = (jax.nn.silu(gate_part) * up_part).astype(jnp.bfloat16)
        return blocked_product(hidden, down_weight, WIDTH_BLOCKS).astype(jnp.bfloat16)
    outputs = lax.map(expert, (buffer, w_gate, w_up, w_down)).reshape(-1, D)
    picked = outputs[destination].astype(jnp.float32).reshape(SEQUENCE_TOKENS, TOP, D)
    mixture = lax.optimization_barrier(jnp.sum(picked * route_weights[:, :, None], axis=1))
    return (stream.astype(jnp.float32) + mixture).astype(jnp.bfloat16)
```

```python
import jax
import jax.numpy as jnp
from jax import lax
from jax.experimental import pallas as pl
from jax.experimental.pallas import tpu as pltpu
from jax.sharding import PartitionSpec as P

HEAD_SIZE = 64
WINDOW = 128
GRID_W = 64


ROPE_BASE = 10000.0
NORM_EPS = 1e-06


def padded(cells, sides, width):
    for axis, dim in sides:
        count = lax.axis_size(axis)
        ends = count - 1
        head = lax.slice_in_dim(cells, 0, width, axis=dim)
        tail = lax.slice_in_dim(cells, cells.shape[dim] - width, cells.shape[dim], axis=dim)
        cells = jnp.concatenate(
            [
                lax.ppermute(tail, axis, [(i, (i + 1) % count) for i in range(ends)]),
                cells,
                lax.ppermute(head, axis, [((i + 1) % count, i) for i in range(ends)]),
            ],
            axis=dim,
        )
    return cells


def rotate_pair(values_half, angles):
    first_half, second = jnp.split(values_half, 2, axis=-1)
    cosine = jnp.cos(angles)[:, None, :]
    sine_part = jnp.sin(angles)[:, None, :]
    return jnp.concatenate(
        [first_half * cosine - second * sine_part, second * cosine + first_half * sine_part],
        axis=-1,
    )


def axial_rotation(heads_in, token_positions):
    half_dim = HEAD_SIZE // 2
    inverse = ROPE_BASE ** (-jnp.arange(0, half_dim, 2, dtype=jnp.float32) / half_dim)
    row_angles = (token_positions // GRID_W).astype(jnp.float32)[:, None] * inverse
    col_angles = (token_positions % GRID_W).astype(jnp.float32)[:, None] * inverse
    as_float = heads_in.astype(jnp.float32)
    return jnp.concatenate(
        [
            rotate_pair(as_float[..., :half_dim], row_angles),
            rotate_pair(as_float[..., half_dim:], col_angles),
        ],
        axis=-1,
    )


def attend_block(query_rows, key_rows, value_rows, sink_logit, query_pos, key_pos, total_rows):
    kv_heads = key_rows.shape[1]
    groups = query_rows.shape[1] // kv_heads
    grouped = query_rows.reshape(query_rows.shape[0], kv_heads, groups, HEAD_SIZE)
    scores = jnp.einsum(
        "qkgd,jkd->kgqj", grouped, key_rows, preferred_element_type=jnp.float32
    ) * HEAD_SIZE ** (-0.5)
    in_window = (
        (jnp.abs(key_pos[None, :] - query_pos[:, None]) <= WINDOW)
        & (key_pos[None, :] >= 0)
        & (key_pos[None, :] < total_rows)
    )
    scores = jnp.where(in_window[None, None], scores, -jnp.inf)
    sink_col = sink_logit.reshape(kv_heads, groups, 1, 1)
    largest = jnp.maximum(jnp.max(scores, axis=-1, keepdims=True), sink_col)
    exp_scores = jnp.exp(scores - largest)
    denominator = jnp.sum(exp_scores, axis=-1, keepdims=True) + jnp.exp(sink_col - largest)
    weights_bf = (exp_scores / denominator).astype(jnp.bfloat16)
    mixed_heads = jnp.einsum(
        "kgqj,jkd->qkgd", weights_bf, value_rows, preferred_element_type=jnp.float32
    )
    return mixed_heads.astype(jnp.bfloat16).reshape(query_rows.shape[0], -1)


MESH = pl.DeviceIdType.MESH
VMEM = pl.BlockSpec(memory_space=pltpu.VMEM)
VMEM_LIMIT = 56 * 1024 * 1024


def tp_places():
    here = lax.axis_index("tp")
    mate = here + 1 - 2 * lax.rem(here, 2)
    across = lax.rem(here + 2, 4)
    return here, mate, across


def send(src, dst, send_sem, recv_sem, sp, tp):
    return pltpu.make_async_remote_copy(
        src_ref=src,
        dst_ref=dst,
        send_sem=send_sem,
        recv_sem=recv_sem,
        device_id=(sp, tp),
        device_id_type=MESH,
    )


def shift_at(step, count):
    return 1 + lax.rem(count // 2 - 1 + step, count - 1)


def greet(count, me, here, mate, across):
    barrier = pltpu.get_barrier_semaphore()

    def signal(shift, carry):
        pl.semaphore_signal(
            barrier, inc=1, device_id=(lax.rem(me + shift, count), here), device_id_type=MESH
        )
        return carry

    lax.fori_loop(1, count, signal, 0)
    for other in (mate, across):
        pl.semaphore_signal(barrier, inc=1, device_id=(me, other), device_id_type=MESH)
    pl.semaphore_wait(barrier, count + 1)


def project_dispatch_kernel(
    count,
    pieces,
    partial,
    residual,
    gain,
    places,
    gathered,
    stream_cols,
    from_mate,
    pair,
    from_across,
    stream,
    normed,
    own,
    mate_sems,
    across_sems,
    back_sems,
    slot_sems,
    near_sems,
    side_sems,
    relay_sems,
    local_sem,
):
    me = lax.axis_index("sp")
    here, mate, across = tp_places()
    half = partial.shape[0] // 2
    rows = half // pieces
    mine = pl.multiple_of(lax.rem(here, 2) * half, rows)
    theirs = pl.multiple_of(half - mine, rows)
    greet(count, me, here, mate, across)

    def to_mate(i):
        return send(
            partial.at[pl.ds(theirs + i * rows, rows)], from_mate.at[pl.ds(i * rows, rows)],
            mate_sems.at[0, i], mate_sems.at[1, i], me, mate,
        )

    def to_across(i):
        return send(
            pair.at[pl.ds(i * rows, rows)], from_across.at[pl.ds(i * rows, rows)],
            across_sems.at[0, i], across_sems.at[1, i], me, across,
        )

    def to_back(i, start):
        part = stream.at[pl.ds(start + i * rows, rows)]
        return send(part, part, back_sems.at[0, i], back_sems.at[1, i], me, mate)

    def normalise(at):
        x = stream[at, :].astype(jnp.float32)
        scale = lax.rsqrt(jnp.mean(x * x, axis=-1, keepdims=True) + NORM_EPS)
        normed[at, :] = (x * scale * gain[...]).astype(jnp.bfloat16)

    for i in range(pieces):
        to_mate(i).start()
    for i in range(pieces):
        to_mate(i).wait_recv()
        at = pl.ds(i * rows, rows)
        pair[at, :] = (
            partial[pl.ds(mine + i * rows, rows), :].astype(jnp.float32)
            + from_mate[at, :].astype(jnp.float32)
        ).astype(jnp.bfloat16)
        to_across(i).start()
    for i in range(pieces):
        to_across(i).wait_recv()
        at = pl.ds(i * rows, rows)
        full = pl.ds(mine + i * rows, rows)
        stream[full, :] = (
            residual[full, :].astype(jnp.float32)
            + (pair[at, :].astype(jnp.float32) + from_across[at, :].astype(jnp.float32))
        ).astype(jnp.bfloat16)
        to_back(i, mine).start()
        normalise(full)
    for i in range(pieces):
        to_back(i, theirs).wait_recv()
        normalise(pl.ds(theirs + i * rows, rows))
    width = stream_cols.shape[1]
    stream_cols[...] = stream[:, pl.ds(pl.multiple_of(here * width, 128), width)]
    quarter = own.shape[1]
    rowid = lax.broadcasted_iota(jnp.int32, (count * quarter, places.shape[1]), 0)
    chosen = (rowid == places[0:1, :]) | (rowid == places[1:2, :])
    chosen = jnp.where(chosen, 1.0, 0.0).astype(jnp.bfloat16)
    picked = jnp.dot(chosen, normed[...], preferred_element_type=jnp.float32).astype(jnp.bfloat16)
    for e in range(count):
        own[e] = picked[e * quarter : (e + 1) * quarter, :]

    def to_expert(k):
        return send(
            own.at[lax.rem(me + k, count)], gathered.at[me, here],
            slot_sems.at[0, k], slot_sems.at[1, k], lax.rem(me + k, count), here,
        )

    def source(k):
        return lax.rem(me - k + count, count)

    def to_near(k, src):
        return send(
            src, gathered.at[source(k), here],
            near_sems.at[0, k], near_sems.at[1, k], me, mate,
        )

    def to_side(k, src):
        return send(
            src, gathered.at[source(k), here],
            side_sems.at[0, k], side_sems.at[1, k], me, across,
        )

    def to_relay(k):
        part = gathered.at[source(k), across]
        return send(part, part, relay_sems.at[0, k], relay_sems.at[1, k], me, mate)

    kept = pltpu.make_async_copy(own.at[me], gathered.at[me, here], local_sem)
    kept.start()

    def start_slot(j, carry):
        to_expert(shift_at(j, count)).start()
        return carry

    to_side(0, own.at[me]).start()
    lax.fori_loop(0, count - 1, start_slot, 0)
    to_near(0, own.at[me]).start()

    def landed(k):
        return gathered.at[source(k), here]

    def pass_on(j, last):
        k = shift_at(j, count)
        to_expert(k).wait_recv()
        to_side(k, landed(k)).start()
        to_near(k, landed(k)).start()
        to_side(last, landed(last)).wait_recv()
        to_relay(last).start()
        return k

    last = lax.fori_loop(0, count - 1, pass_on, 0)
    to_side(last, landed(last)).wait_recv()
    to_relay(last).start()

    def finish(k, carry):
        to_near(k, landed(k)).wait()
        to_relay(k).wait()
        to_side(k, landed(k)).wait_send()
        return carry

    lax.fori_loop(0, count, finish, 0)

    def finish_slot(k, carry):
        to_expert(k).wait_send()
        return carry

    lax.fori_loop(1, count, finish_slot, 0)
    kept.wait()
    for i in range(pieces):
        to_mate(i).wait_send()
        to_across(i).wait_send()
        to_back(i, mine).wait_send()


def project_dispatch(partial, residual, gain, places, count, quarter, cols, pieces):
    rows, width = partial.shape
    half = rows // 2
    dma = pltpu.SemaphoreType.DMA
    bf = jnp.bfloat16
    return pl.pallas_call(
        lambda *refs: project_dispatch_kernel(count, pieces, *refs),
        out_shape=(
            jax.ShapeDtypeStruct((count, 4, quarter, width), bf),
            jax.ShapeDtypeStruct((rows, cols), bf),
        ),
        in_specs=[VMEM] * 4,
        out_specs=(VMEM, VMEM),
        scratch_shapes=[
            pltpu.VMEM((half, width), bf),
            pltpu.VMEM((half, width), bf),
            pltpu.VMEM((half, width), bf),
            pltpu.VMEM((rows, width), bf),
            pltpu.VMEM((rows, width), bf),
            pltpu.VMEM((count, quarter, width), bf),
            dma((2, pieces)),
            dma((2, pieces)),
            dma((2, pieces)),
            dma((2, count)),
            dma((2, count)),
            dma((2, count)),
            dma((2, count)),
            dma,
        ],
        compiler_params=pltpu.CompilerParams(
            collective_id=0, has_side_effects=True, vmem_limit_bytes=VMEM_LIMIT
        ),
    )(partial, residual, gain, places)


def combine_kernel(
    count,
    partial,
    stream_cols,
    target,
    weight,
    out,
    from_mate,
    pair,
    from_across,
    total,
    back,
    mix,
    mate_sems,
    across_sems,
    back_sems,
    local_sem,
):
    me = lax.axis_index("sp")
    here, mate, across = tp_places()
    cols = out.shape[1]
    slots = partial.shape[1]
    greet(count, me, here, mate, across)

    def block(which):
        return pl.ds(pl.multiple_of(which * cols, 128), cols)

    def dest(k):
        return lax.rem(me + k, count)

    def order(j):
        return lax.rem(count // 2 + j, count)

    def to_mate(k, part):
        cb = mate if part == 0 else lax.rem(mate + 2, 4)
        return send(
            partial.at[dest(k), :, block(cb)], from_mate.at[dest(k), part],
            mate_sems.at[0, part, k], mate_sems.at[1, part, k], me, mate,
        )

    def to_across(k):
        return send(
            pair.at[dest(k)], from_across.at[dest(k)],
            across_sems.at[0, k], across_sems.at[1, k], me, across,
        )

    def to_back(k):
        return send(
            total.at[dest(k)], back.at[me], back_sems.at[0, k], back_sems.at[1, k], dest(k), here
        )

    def start_mate(j, carry):
        to_mate(order(j), 1).start()
        to_mate(order(j), 0).start()
        return carry

    lax.fori_loop(0, count, start_mate, 0)

    def start_across(j, carry):
        k = order(j)
        to_mate(k, 1).wait_recv()
        pair[dest(k)] = (
            partial[dest(k), :, block(across)].astype(jnp.float32)
            + from_mate[dest(k), 1].astype(jnp.float32)
        ).astype(jnp.bfloat16)
        to_across(k).start()
        return carry

    lax.fori_loop(0, count, start_across, 0)

    def start_back(j, carry):
        k = order(j)
        to_mate(k, 0).wait_recv()
        to_across(k).wait_recv()
        total[dest(k)] = (
            partial[dest(k), :, block(here)].astype(jnp.float32)
            + from_mate[dest(k), 0].astype(jnp.float32)
            + from_across[dest(k)].astype(jnp.float32)
        ).astype(jnp.bfloat16)

        @pl.when(k != 0)
        def _():
            to_back(k).start()

        return carry

    lax.fori_loop(0, count, start_back, 0)
    kept = pltpu.make_async_copy(total.at[me], back.at[me], local_sem)
    kept.start()
    mix[...] = jnp.zeros_like(mix)
    slot_ids = lax.broadcasted_iota(jnp.int32, (out.shape[0], slots), 1)

    def add(expert):
        ids = slot_ids + expert * slots
        table = jnp.where(ids == target[:, 0:1], weight[:, 0:1], 0.0) + jnp.where(
            ids == target[:, 1:2], weight[:, 1:2], 0.0
        )
        high = table.astype(jnp.bfloat16)
        low = (table - high.astype(jnp.float32)).astype(jnp.bfloat16)
        rows = back[expert]
        mix[...] += jnp.dot(high, rows, preferred_element_type=jnp.float32) + jnp.dot(
            low, rows, preferred_element_type=jnp.float32
        )

    kept.wait()
    add(me)

    def receive(j, carry):
        k = shift_at(j, count)
        to_back(k).wait_recv()
        add(lax.rem(me - k + count, count))
        return carry

    lax.fori_loop(0, count - 1, receive, 0)
    out[...] = (stream_cols[...].astype(jnp.float32) + mix[...]).astype(jnp.bfloat16)

    def finish(k, carry):
        to_mate(k, 0).wait_send()
        to_mate(k, 1).wait_send()
        to_across(k).wait_send()
        return carry

    lax.fori_loop(0, count, finish, 0)

    def finish_back(k, carry):
        to_back(k).wait_send()
        return carry

    lax.fori_loop(1, count, finish_back, 0)


def combine(partial, stream_cols, target, weight):
    count, slots, _ = partial.shape
    cols = stream_cols.shape[1]
    dma = pltpu.SemaphoreType.DMA
    bf = jnp.bfloat16
    return pl.pallas_call(
        lambda *refs: combine_kernel(count, *refs),
        out_shape=jax.ShapeDtypeStruct(stream_cols.shape, bf),
        in_specs=[VMEM] * 4,
        out_specs=VMEM,
        scratch_shapes=[
            pltpu.VMEM((count, 2, slots, cols), bf),
            pltpu.VMEM((count, slots, cols), bf),
            pltpu.VMEM((count, slots, cols), bf),
            pltpu.VMEM((count, slots, cols), bf),
            pltpu.VMEM((count, slots, cols), bf),
            pltpu.VMEM(stream_cols.shape, jnp.float32),
            dma((2, 2, count)),
            dma((2, count)),
            dma((2, count)),
            dma,
        ],
        compiler_params=pltpu.CompilerParams(
            collective_id=1, has_side_effects=True, vmem_limit_bytes=VMEM_LIMIT
        ),
    )(partial, stream_cols, target, weight)


def local(
    query_proj,
    key_projection,
    value_projection,
    sink_logit,
    residual,
    w_out,
    norm_gain,
    routes,
    route_weights,
    w_gate,
    w_up,
    w_down,
):
    tok_rows = query_proj.shape[0]
    seq_devices = lax.axis_size("sp")
    total_rows = tok_rows * seq_devices
    offset = lax.axis_index("sp") * tok_rows
    kv_width = key_projection.shape[1]
    joined = jnp.concatenate([key_projection, value_projection], axis=1)
    widened = padded(joined, (("sp", 0),), WINDOW)
    query_pos = offset + jnp.arange(tok_rows, dtype=jnp.int32)
    key_pos = offset - WINDOW + jnp.arange(tok_rows + 2 * WINDOW, dtype=jnp.int32)
    rot_q = axial_rotation(query_proj.reshape(tok_rows, -1, HEAD_SIZE), query_pos).astype(
        jnp.bfloat16
    )
    rotated_keys = axial_rotation(
        widened[:, :kv_width].reshape(-1, kv_width // HEAD_SIZE, HEAD_SIZE), key_pos
    ).astype(jnp.bfloat16)
    value_head_rows = widened[:, kv_width:].reshape(-1, kv_width // HEAD_SIZE, HEAD_SIZE)
    attended = attend_block(
        rot_q, rotated_keys, value_head_rows, sink_logit, query_pos, key_pos, total_rows
    )
    partial_value = jnp.dot(attended, w_out, preferred_element_type=jnp.float32)
    width = partial_value.shape[1]
    col_blocks = lax.axis_size("tp")
    col_width = width // col_blocks
    top_count = routes.shape[1]
    experts = w_gate.shape[0] * seq_devices
    capacity = 2 * top_count * tok_rows // experts
    quarter = capacity // col_blocks
    expert_ids = jnp.arange(experts, dtype=jnp.int32)
    named = routes[:, :, None] == expert_ids
    counted = jnp.any(named, axis=1).astype(jnp.bfloat16)
    earlier = jnp.tri(tok_rows, k=-1, dtype=jnp.bfloat16)
    before = jnp.dot(earlier, counted, preferred_element_type=jnp.float32)
    slot_number = jnp.sum(jnp.where(named, before[:, None, :], 0.0), axis=2).astype(jnp.int32)
    destination = routes * capacity + slot_number
    inside = slot_number - lax.axis_index("tp") * quarter
    places = jnp.where((inside >= 0) & (inside < quarter), routes * quarter + inside, -1).T
    gathered, stream_cols = project_dispatch(
        partial_value.astype(jnp.bfloat16), residual, norm_gain[None, :], places,
        seq_devices, quarter, col_width, 4,
    )
    expert_rows = gathered.reshape(-1, width)
    gate_part = jnp.dot(expert_rows, w_gate[0], preferred_element_type=jnp.float32)
    up_part = jnp.dot(expert_rows, w_up[0], preferred_element_type=jnp.float32)
    hidden = (jax.nn.silu(gate_part) * up_part).astype(jnp.bfloat16)
    partial_rows = jnp.dot(hidden, w_down[0], preferred_element_type=jnp.float32)
    return combine(
        partial_rows.astype(jnp.bfloat16).reshape(seq_devices, capacity, width),
        stream_cols, destination, route_weights,
    )


def solution(mesh):
    return jax.shard_map(
        local,
        mesh=mesh,
        in_specs=(
            P("sp", "tp"),
            P("sp", "tp"),
            P("sp", "tp"),
            P("tp"),
            P("sp", None),
            P("tp", None),
            P(),
            P("sp", None),
            P("sp", None),
            P("sp", None, "tp"),
            P("sp", None, "tp"),
            P("sp", "tp", None),
        ),
        out_specs=P("sp", "tp"),
        check_vma=False,
    )
```

```python
import jax
import jax.numpy as jnp
from jax import lax
from jax.experimental import pallas as pl
from jax.experimental.pallas import tpu as pltpu
from jax.sharding import PartitionSpec as P

HEAD_SIZE = 64
WINDOW = 128
GRID_W = 64


ROPE_BASE = 10000.0
NORM_EPS = 1e-06


MESH = pl.DeviceIdType.MESH
VMEM = pl.BlockSpec(memory_space=pltpu.VMEM)
VMEM_LIMIT = 56 * 1024 * 1024


def tp_places():
    here = lax.axis_index("tp")
    mate = here + 1 - 2 * lax.rem(here, 2)
    across = lax.rem(here + 2, 4)
    return here, mate, across


def send(src, dst, send_sem, recv_sem, sp, tp):
    return pltpu.make_async_remote_copy(
        src_ref=src,
        dst_ref=dst,
        send_sem=send_sem,
        recv_sem=recv_sem,
        device_id=(sp, tp),
        device_id_type=MESH,
    )


def shift_at(step, count):
    return 1 + lax.rem(count // 2 - 1 + step, count - 1)


def greet(count, me, here, mate, across):
    barrier = pltpu.get_barrier_semaphore()

    def signal(shift, carry):
        pl.semaphore_signal(
            barrier, inc=1, device_id=(lax.rem(me + shift, count), here), device_id_type=MESH
        )
        return carry

    lax.fori_loop(1, count, signal, 0)
    for other in (mate, across):
        pl.semaphore_signal(barrier, inc=1, device_id=(me, other), device_id_type=MESH)
    pl.semaphore_wait(barrier, count + 1)


def project_dispatch_kernel(
    count,
    pieces,
    sinks,
    query,
    keys,
    values,
    row_turn,
    col_turn,
    swap,
    gain,
    routes,
    w_out_hbm,
    residual_hbm,
    w_gate_hbm,
    w_up_hbm,
    hidden,
    stream_cols,
    target,
    gathered,
    w_gate,
    w_up,
    key_wide,
    value_wide,
    key_twice,
    value_twice,
    turned,
    attended,
    w_out,
    residual,
    partial,
    from_mate,
    pair,
    from_across,
    stream,
    normed,
    own,
    mate_sems,
    across_sems,
    back_sems,
    slot_sems,
    near_sems,
    side_sems,
    relay_sems,
    local_sem,
    halo_sems,
    load_sems,
):
    me = lax.axis_index("sp")
    here, mate, across = tp_places()
    half = partial.shape[0] // 2
    rows = half // pieces
    mine = pl.multiple_of(lax.rem(here, 2) * half, rows)
    theirs = pl.multiple_of(half - mine, rows)
    loads = [
        pltpu.make_async_copy(w_out_hbm, w_out, load_sems.at[0]),
        pltpu.make_async_copy(residual_hbm, residual, load_sems.at[1]),
        pltpu.make_async_copy(w_gate_hbm, w_gate, load_sems.at[2]),
        pltpu.make_async_copy(w_up_hbm, w_up, load_sems.at[3]),
    ]
    for load in loads:
        load.start()
    greet(count, me, here, mate, across)
    tokens = query.shape[0]
    up, down = me + 1, me - 1
    low, high = pl.ds(0, WINDOW), pl.ds(tokens + WINDOW, WINDOW)
    pairs = ((keys, key_wide), (values, value_wide))

    def halo(which, upward):
        raw, wide = pairs[which]
        if upward:
            src, dst, sp = raw.at[pl.ds(tokens - WINDOW, WINDOW)], wide.at[low], up
        else:
            src, dst, sp = raw.at[pl.ds(0, WINDOW)], wide.at[high], down
        way = 1 if upward else 0
        return send(src, dst, halo_sems.at[0, which, way], halo_sems.at[1, which, way], sp, here)

    @pl.when(me < count - 1)
    def _():
        halo(0, True).start()
        halo(1, True).start()

    @pl.when(me > 0)
    def _():
        halo(0, False).start()
        halo(1, False).start()

    lane = lax.broadcasted_iota(jnp.int32, (1, 128), 1)
    by_row = lax.rem(lane, HEAD_SIZE) < HEAD_SIZE // 2
    left = lane < HEAD_SIZE
    edge = WINDOW // GRID_W

    def turn(x, grid_row):
        cosine = jnp.where(by_row, row_turn[0, grid_row : grid_row + 1, :], col_turn[0])
        sine = jnp.where(by_row, row_turn[1, grid_row : grid_row + 1, :], col_turn[1])
        swapped = jnp.dot(x, swap[...], preferred_element_type=jnp.float32)
        return (x.astype(jnp.float32) * cosine + swapped * sine).astype(jnp.bfloat16)

    def twice(x, place, at):
        other = pltpu.roll(x.astype(jnp.float32), HEAD_SIZE, 1).astype(jnp.bfloat16)
        place[0, at, :] = jnp.where(left, x, other)
        place[1, at, :] = jnp.where(left, other, x)

    for r in range(tokens // GRID_W):
        at = pl.ds(r * GRID_W, GRID_W)
        for j in range(query.shape[1] // 128):
            block = pl.ds(j * 128, 128)
            turned[at, block] = turn(query[at, block], r + edge) * HEAD_SIZE**-0.5
        wide_at = pl.ds(WINDOW + r * GRID_W, GRID_W)
        twice(turn(keys[at, :], r + edge), key_twice, wide_at)
        twice(values[at, :], value_twice, wide_at)

    @pl.when(me > 0)
    def _():
        halo(0, True).wait_recv()
        halo(1, True).wait_recv()

    @pl.when(me == 0)
    def _():
        key_wide[low, :] = jnp.zeros((WINDOW, 128), jnp.bfloat16)
        value_wide[low, :] = jnp.zeros((WINDOW, 128), jnp.bfloat16)

    @pl.when(me < count - 1)
    def _():
        halo(0, False).wait_recv()
        halo(1, False).wait_recv()

    @pl.when(me == count - 1)
    def _():
        key_wide[high, :] = jnp.zeros((WINDOW, 128), jnp.bfloat16)
        value_wide[high, :] = jnp.zeros((WINDOW, 128), jnp.bfloat16)

    for r in range(edge):
        for g in (r, edge + tokens // GRID_W + r):
            at = pl.ds(g * GRID_W, GRID_W)
            twice(turn(key_wide[at, :], g), key_twice, at)
            twice(value_wide[at, :], value_twice, at)

    reach = half + 2 * WINDOW
    gap = lax.broadcasted_iota(jnp.int32, (half, reach), 1) - lax.broadcasted_iota(
        jnp.int32, (half, reach), 0
    )
    spot = lax.broadcasted_iota(jnp.int32, (half, reach), 1)
    groups = query.shape[1] // keys.shape[1]

    def attend(first):
        place = spot + (me * tokens + first - WINDOW)
        kept = (gap >= 0) & (gap <= 2 * WINDOW) & (place >= 0) & (place < count * tokens)
        both = jnp.concatenate([kept, kept], axis=0)
        near = pl.ds(first, reach)
        top = lax.broadcasted_iota(jnp.int32, (2 * half, 1), 0) < half
        for j in range(query.shape[1] // 128):
            head = 2 * j // groups
            q = turned[pl.ds(first, half), pl.ds(j * 128, 128)]
            none = jnp.zeros_like(q)
            q = jnp.concatenate([jnp.where(left, q, none), jnp.where(left, none, q)], axis=0)
            scores = lax.dot_general(
                q, key_twice[head, near, :], (((1,), (1,)), ((), ())),
                preferred_element_type=jnp.float32,
            )
            scores = jnp.where(both, scores, -jnp.inf)
            sink = jnp.where(top, sinks[2 * j], sinks[2 * j + 1])
            largest = jnp.maximum(jnp.max(scores, axis=-1, keepdims=True), sink)
            grown = jnp.exp(scores - largest)
            below = jnp.sum(grown, axis=-1, keepdims=True) + jnp.exp(sink - largest)
            probs = (grown * (1.0 / below)).astype(jnp.bfloat16)
            mixed = jnp.dot(probs, value_twice[head, near, :], preferred_element_type=jnp.float32)
            attended[:, pl.ds(j * 128, 128)] = jnp.where(
                left, mixed[:half], mixed[half:]
            ).astype(jnp.bfloat16)
        partial[pl.ds(first, half), :] = jnp.dot(
            attended[...], w_out[...], preferred_element_type=jnp.float32
        ).astype(jnp.bfloat16)

    def to_mate(i):
        return send(
            partial.at[pl.ds(theirs + i * rows, rows)], from_mate.at[pl.ds(i * rows, rows)],
            mate_sems.at[0, i], mate_sems.at[1, i], me, mate,
        )

    def to_across(i):
        return send(
            pair.at[pl.ds(i * rows, rows)], from_across.at[pl.ds(i * rows, rows)],
            across_sems.at[0, i], across_sems.at[1, i], me, across,
        )

    def to_back(i, start):
        part = stream.at[pl.ds(start + i * rows, rows)]
        return send(part, part, back_sems.at[0, i], back_sems.at[1, i], me, mate)

    def normalise(at):
        x = stream[at, :].astype(jnp.float32)
        scale = lax.rsqrt(jnp.mean(x * x, axis=-1, keepdims=True) + NORM_EPS)
        normed[at, :] = (x * scale * gain[...]).astype(jnp.bfloat16)

    loads[0].wait()
    attend(theirs)
    for i in range(pieces):
        to_mate(i).start()
    attend(mine)
    loads[1].wait()
    for i in range(pieces):
        to_mate(i).wait_recv()
        at = pl.ds(i * rows, rows)
        pair[at, :] = (
            partial[pl.ds(mine + i * rows, rows), :].astype(jnp.float32)
            + from_mate[at, :].astype(jnp.float32)
        ).astype(jnp.bfloat16)
        to_across(i).start()
    quarter = own.shape[1]
    lanes = -(-count // 128) * 128
    expert_ids = lax.broadcasted_iota(jnp.int32, (tokens, lanes), 1)
    names = [routes[:, k : k + 1] == expert_ids for k in range(2)]
    counted = jnp.where(names[0] | names[1], 1.0, 0.0).astype(jnp.bfloat16)
    older = lax.broadcasted_iota(jnp.int32, (tokens, tokens), 1) < lax.broadcasted_iota(
        jnp.int32, (tokens, tokens), 0
    )
    before = jnp.dot(
        jnp.where(older, 1.0, 0.0).astype(jnp.bfloat16), counted,
        preferred_element_type=jnp.float32,
    )
    slot_ids = lax.broadcasted_iota(jnp.int32, (tokens, count * quarter), 1)
    slot_ids = slot_ids.astype(jnp.float32)
    begin = (here * quarter).astype(jnp.float32)
    chosen = jnp.zeros((tokens, count * quarter), jnp.float32)
    for k in range(2):
        slot = jnp.sum(jnp.where(names[k], before, 0.0), axis=1, keepdims=True)
        expert = routes[:, k : k + 1].astype(jnp.float32)
        target[:, k : k + 1] = expert * (4 * quarter) + slot
        inside = slot - begin
        fits = (inside >= 0.0) & (inside < quarter)
        row = jnp.where(fits, expert * quarter + inside, -1.0)
        chosen = jnp.where(slot_ids == row, 1.0, chosen)
    chosen = chosen.astype(jnp.bfloat16)
    for i in range(pieces):
        to_across(i).wait_recv()
        at = pl.ds(i * rows, rows)
        full = pl.ds(mine + i * rows, rows)
        stream[full, :] = (
            residual[full, :].astype(jnp.float32)
            + (pair[at, :].astype(jnp.float32) + from_across[at, :].astype(jnp.float32))
        ).astype(jnp.bfloat16)
        to_back(i, mine).start()
        normalise(full)
    for i in range(pieces):
        to_back(i, theirs).wait_recv()
        normalise(pl.ds(theirs + i * rows, rows))
    width = stream_cols.shape[1]
    stream_cols[...] = stream[:, pl.ds(pl.multiple_of(here * width, 128), width)]
    picked = lax.dot_general(
        chosen, normed[...], (((0,), (0,)), ((), ())), preferred_element_type=jnp.float32
    ).astype(jnp.bfloat16)
    for e in range(count):
        own[e] = picked[e * quarter : (e + 1) * quarter, :]

    def to_expert(k):
        return send(
            own.at[lax.rem(me + k, count)], gathered.at[me, here],
            slot_sems.at[0, k], slot_sems.at[1, k], lax.rem(me + k, count), here,
        )

    def source(k):
        return lax.rem(me - k + count, count)

    def to_near(k, src):
        return send(
            src, gathered.at[source(k), here],
            near_sems.at[0, k], near_sems.at[1, k], me, mate,
        )

    def to_side(k, src):
        return send(
            src, gathered.at[source(k), here],
            side_sems.at[0, k], side_sems.at[1, k], me, across,
        )

    def to_relay(k):
        part = gathered.at[source(k), across]
        return send(part, part, relay_sems.at[0, k], relay_sems.at[1, k], me, mate)

    kept = pltpu.make_async_copy(own.at[me], gathered.at[me, here], local_sem)
    kept.start()

    def start_slot(j, carry):
        to_expert(shift_at(j, count)).start()
        return carry

    to_side(0, own.at[me]).start()
    lax.fori_loop(0, count - 1, start_slot, 0)
    to_near(0, own.at[me]).start()

    def landed(k):
        return gathered.at[source(k), here]

    def expert_rows(k):
        parts = [gathered[source(k), q] for q in range(4)]
        if quarter % 16:
            parts = [part.astype(jnp.float32) for part in parts]
        rows_in = jnp.concatenate(parts, axis=0).astype(jnp.bfloat16)
        gate = jnp.dot(rows_in, w_gate[...], preferred_element_type=jnp.float32)
        raised = jnp.dot(rows_in, w_up[...], preferred_element_type=jnp.float32)
        hidden[source(k)] = (jax.nn.silu(gate) * raised).astype(jnp.bfloat16)

    def settle(k):
        to_near(k, landed(k)).wait_recv()
        to_relay(k).wait_recv()
        expert_rows(k)

    def pass_on(j, carry):
        last, older = carry
        k = shift_at(j, count)
        to_expert(k).wait_recv()
        to_side(k, landed(k)).start()
        to_near(k, landed(k)).start()
        to_side(last, landed(last)).wait_recv()
        to_relay(last).start()

        @pl.when(j > 0)
        def _():
            settle(older)

        return k, last

    for load in loads[2:]:
        load.wait()
    kept.wait()
    last, older = lax.fori_loop(0, count - 1, pass_on, (0, 0))
    settle(older)
    to_side(last, landed(last)).wait_recv()
    to_relay(last).start()
    settle(last)

    def finish(k, carry):
        to_near(k, landed(k)).wait_send()
        to_relay(k).wait_send()
        to_side(k, landed(k)).wait_send()
        return carry

    lax.fori_loop(0, count, finish, 0)

    def finish_slot(k, carry):
        to_expert(k).wait_send()
        return carry

    lax.fori_loop(1, count, finish_slot, 0)
    for i in range(pieces):
        to_mate(i).wait_send()
        to_across(i).wait_send()
        to_back(i, mine).wait_send()

    @pl.when(me < count - 1)
    def _():
        halo(0, True).wait_send()
        halo(1, True).wait_send()

    @pl.when(me > 0)
    def _():
        halo(0, False).wait_send()
        halo(1, False).wait_send()


def project_dispatch(operands, count, quarter, cols, pieces):
    query, keys = operands[1], operands[2]
    w_out, residual, w_gate, w_up = operands[-4:]
    rows, width = residual.shape
    half = rows // 2
    wide = (rows + 2 * WINDOW, keys.shape[1])
    dma = pltpu.SemaphoreType.DMA
    bf = jnp.bfloat16
    return pl.pallas_call(
        lambda *refs: project_dispatch_kernel(count, pieces, *refs),
        out_shape=(
            jax.ShapeDtypeStruct((count, 4 * quarter, w_up.shape[1]), bf),
            jax.ShapeDtypeStruct((rows, cols), bf),
            jax.ShapeDtypeStruct((rows, 2), jnp.float32),
        ),
        in_specs=[pl.BlockSpec(memory_space=pltpu.SMEM)]
        + [VMEM] * 8
        + [pl.BlockSpec(memory_space=pl.ANY)] * 4,
        out_specs=(VMEM, VMEM, VMEM),
        scratch_shapes=[
            pltpu.VMEM((count, 4, quarter, width), bf),
            pltpu.VMEM(w_gate.shape, bf),
            pltpu.VMEM(w_up.shape, bf),
            pltpu.VMEM(wide, bf),
            pltpu.VMEM(wide, bf),
            pltpu.VMEM((2, *wide), bf),
            pltpu.VMEM((2, *wide), bf),
            pltpu.VMEM(query.shape, bf),
            pltpu.VMEM((half, query.shape[1]), bf),
            pltpu.VMEM(w_out.shape, bf),
            pltpu.VMEM((rows, width), bf),
            pltpu.VMEM((rows, width), bf),
            pltpu.VMEM((half, width), bf),
            pltpu.VMEM((half, width), bf),
            pltpu.VMEM((half, width), bf),
            pltpu.VMEM((rows, width), bf),
            pltpu.VMEM((rows, width), bf),
            pltpu.VMEM((count, quarter, width), bf),
            dma((2, pieces)),
            dma((2, pieces)),
            dma((2, pieces)),
            dma((2, count)),
            dma((2, count)),
            dma((2, count)),
            dma((2, count)),
            dma,
            dma((2, 2, 2)),
            dma((4,)),
        ],
        compiler_params=pltpu.CompilerParams(
            collective_id=0, has_side_effects=True, vmem_limit_bytes=VMEM_LIMIT
        ),
    )(*operands)


def combine_kernel(
    count,
    hidden,
    w_down,
    stream_cols,
    target,
    weight,
    out,
    partial,
    from_mate,
    pair,
    from_across,
    total,
    back,
    mix,
    mate_sems,
    across_sems,
    back_sems,
    local_sem,
):
    me = lax.axis_index("sp")
    here, mate, across = tp_places()
    cols = out.shape[1]
    slots = partial.shape[1]
    greet(count, me, here, mate, across)

    def block(which):
        return pl.ds(pl.multiple_of(which * cols, 128), cols)

    def dest(k):
        return lax.rem(me + k, count)

    def order(j):
        return lax.rem(count // 2 + j, count)

    def to_mate(k, part):
        cb = mate if part == 0 else lax.rem(mate + 2, 4)
        return send(
            partial.at[dest(k), :, block(cb)], from_mate.at[dest(k), part],
            mate_sems.at[0, part, k], mate_sems.at[1, part, k], me, mate,
        )

    def to_across(k):
        return send(
            pair.at[dest(k)], from_across.at[dest(k)],
            across_sems.at[0, k], across_sems.at[1, k], me, across,
        )

    def to_back(k):
        return send(
            total.at[dest(k)], back.at[me], back_sems.at[0, k], back_sems.at[1, k], dest(k), here
        )

    def start_mate(j, carry):
        partial[dest(order(j))] = jnp.dot(
            hidden[dest(order(j))], w_down[...], preferred_element_type=jnp.float32
        ).astype(jnp.bfloat16)
        to_mate(order(j), 1).start()
        to_mate(order(j), 0).start()
        return carry

    def start_across(j, carry):
        k = order(j)
        to_mate(k, 1).wait_recv()
        pair[dest(k)] = (
            partial[dest(k), :, block(across)].astype(jnp.float32)
            + from_mate[dest(k), 1].astype(jnp.float32)
        ).astype(jnp.bfloat16)
        to_across(k).start()
        return carry

    def lead(j, carry):
        start_mate(j + 1, carry)
        return start_across(j, carry)

    start_mate(0, 0)
    lax.fori_loop(0, count - 1, lead, 0)
    start_across(count - 1, 0)

    def start_back(j, carry):
        k = order(j)
        to_mate(k, 0).wait_recv()
        to_across(k).wait_recv()
        total[dest(k)] = (
            partial[dest(k), :, block(here)].astype(jnp.float32)
            + from_mate[dest(k), 0].astype(jnp.float32)
            + from_across[dest(k)].astype(jnp.float32)
        ).astype(jnp.bfloat16)

        @pl.when(k != 0)
        def _():
            to_back(k).start()

        return carry

    lax.fori_loop(0, count, start_back, 0)
    kept = pltpu.make_async_copy(total.at[me], back.at[me], local_sem)
    kept.start()
    mix[...] = jnp.zeros_like(mix)
    slot_ids = lax.broadcasted_iota(jnp.int32, (out.shape[0], slots), 1)
    slot_ids = slot_ids.astype(jnp.float32)

    def add(expert):
        ids = slot_ids + (expert * slots).astype(jnp.float32)
        table = jnp.where(ids == target[:, 0:1], weight[:, 0:1], 0.0) + jnp.where(
            ids == target[:, 1:2], weight[:, 1:2], 0.0
        )
        high = table.astype(jnp.bfloat16)
        low = (table - high.astype(jnp.float32)).astype(jnp.bfloat16)
        rows = back[expert]
        mix[...] += jnp.dot(high, rows, preferred_element_type=jnp.float32) + jnp.dot(
            low, rows, preferred_element_type=jnp.float32
        )

    kept.wait()
    add(me)

    def receive(j, carry):
        k = shift_at(j, count)
        to_back(k).wait_recv()
        add(lax.rem(me - k + count, count))
        return carry

    lax.fori_loop(0, count - 1, receive, 0)
    out[...] = (stream_cols[...].astype(jnp.float32) + mix[...]).astype(jnp.bfloat16)

    def finish(k, carry):
        to_mate(k, 0).wait_send()
        to_mate(k, 1).wait_send()
        to_across(k).wait_send()
        return carry

    lax.fori_loop(0, count, finish, 0)

    def finish_back(k, carry):
        to_back(k).wait_send()
        return carry

    lax.fori_loop(1, count, finish_back, 0)


def combine(hidden, w_down, stream_cols, target, weight):
    count, slots, _ = hidden.shape
    cols = stream_cols.shape[1]
    dma = pltpu.SemaphoreType.DMA
    bf = jnp.bfloat16
    return pl.pallas_call(
        lambda *refs: combine_kernel(count, *refs),
        out_shape=jax.ShapeDtypeStruct(stream_cols.shape, bf),
        in_specs=[VMEM] * 5,
        out_specs=VMEM,
        scratch_shapes=[
            pltpu.VMEM((count, slots, w_down.shape[1]), bf),
            pltpu.VMEM((count, 2, slots, cols), bf),
            pltpu.VMEM((count, slots, cols), bf),
            pltpu.VMEM((count, slots, cols), bf),
            pltpu.VMEM((count, slots, cols), bf),
            pltpu.VMEM((count, slots, cols), bf),
            pltpu.VMEM(stream_cols.shape, jnp.float32),
            dma((2, 2, count)),
            dma((2, count)),
            dma((2, count)),
            dma,
        ],
        compiler_params=pltpu.CompilerParams(
            collective_id=1, has_side_effects=True, vmem_limit_bytes=VMEM_LIMIT
        ),
    )(hidden, w_down, stream_cols, target, weight)


def local(
    query_proj,
    key_projection,
    value_projection,
    sink_logit,
    residual,
    w_out,
    norm_gain,
    routes,
    route_weights,
    w_gate,
    w_up,
    w_down,
):
    tok_rows, _ = query_proj.shape
    width = residual.shape[1]
    seq_devices = lax.axis_size("sp")
    col_blocks = lax.axis_size("tp")
    col_width = width // col_blocks
    experts = w_gate.shape[0] * seq_devices
    capacity = 2 * routes.shape[1] * tok_rows // experts
    quarter = capacity // col_blocks
    half_dim = HEAD_SIZE // 2
    inverse = ROPE_BASE ** (-jnp.arange(0, half_dim, 2, dtype=jnp.float32) / half_dim)
    lane_rates = jnp.tile(inverse, 128 // inverse.shape[0])
    lane = jnp.arange(128)
    first = lane % half_dim < half_dim // 2
    partner = jnp.where(first, lane + half_dim // 2, lane - half_dim // 2)
    swap = jnp.where(
        lane[:, None] == partner[None, :], jnp.where(first, -1.0, 1.0)[None, :], 0.0
    ).astype(jnp.bfloat16)
    grid_rows = (tok_rows + 2 * WINDOW) // GRID_W
    first_row = lax.axis_index("sp") * (tok_rows // GRID_W) - WINDOW // GRID_W
    row_angles = (first_row + jnp.arange(grid_rows)).astype(jnp.float32)[:, None] * lane_rates
    col_angles = jnp.arange(GRID_W, dtype=jnp.float32)[:, None] * lane_rates
    row_turn = jnp.stack([jnp.cos(row_angles), jnp.sin(row_angles)])
    col_turn = jnp.stack([jnp.cos(col_angles), jnp.sin(col_angles)])
    hidden, stream_cols, destination = project_dispatch(
        (
            sink_logit, query_proj, key_projection, value_projection, row_turn, col_turn, swap,
            norm_gain[None, :], routes, w_out, residual, w_gate[0], w_up[0],
        ),
        seq_devices, quarter, col_width, 4,
    )
    return combine(hidden, w_down[0], stream_cols, destination, route_weights)


def solution(mesh):
    return jax.shard_map(
        local,
        mesh=mesh,
        in_specs=(
            P("sp", "tp"),
            P("sp", "tp"),
            P("sp", "tp"),
            P("tp"),
            P("sp", None),
            P("tp", None),
            P(),
            P("sp", None),
            P("sp", None),
            P("sp", None, "tp"),
            P("sp", None, "tp"),
            P("sp", "tp", None),
        ),
        out_specs=P("sp", "tp"),
        check_vma=False,
    )
```
